32 devices in a mesh: ep: 8 (over z, x), tp: 4 (over y, core).
Axes of the slice: x: 2, y: 2, z: 4, core: 2. Of those that a mesh axis runs over, the one named last changes fastest.
Arguments:
- queries: bfloat16 [2048, 1024], P('ep', 'tp'), may hold values from -5 to 5
- keys: bfloat16 [2048, 1024], P('ep', 'tp'), may hold values from -5 to 5
- values: bfloat16 [2048, 1024], P('ep', 'tp'), may hold values from -6 to 6
- gate_totals: float32 [2048, 8], P('ep', 'tp'), as said below
- out_proj: bfloat16 [1024, 2048], P('tp'), may hold values from -0.75 to 0.75
- moe_input: bfloat16 [3072, 2048], P('ep'), may hold values from -600 to 600
- norm_gain: float32 [2048], replicated, may hold values from 0.1 to 1.9
- routes: int32 [3072, 2], P('ep'), may hold values from 0 to 7, all different within a row; in each aligned block of 384 rows (0 to 383, 384 to 767, ...) at most 100 rows name the same one
- route_logits: float32 [3072, 2], P('ep'), may hold values from -6 to 6
- expert_gate: bfloat16 [8, 2048, 3072], P('ep', None, 'tp'), may hold values from -0.125 to 0.125
- expert_up: bfloat16 [8, 2048, 3072], P('ep', None, 'tp'), may hold values from -0.125 to 0.125
- expert_down: bfloat16 [8, 3072, 2048], P('ep', 'tp'), may hold values from -0.109375 to 0.109375
Outputs:
- mixed: bfloat16 [2048, 2048], P('ep', 'tp')
- routed: bfloat16 [3072, 2048], P('ep', 'tp')
The draws below stay inside these ranges and needn't reach their ends.
Inputs may be any that keep to these rules, and one draw needn't show every extreme that they name: `gate_totals`: along the positions, each head's values never increase. `routes`: A token names 2 different experts. Among the 384 tokens of one index of ep no expert is named more than 100 times, and in some of these blocks one expert is named exactly 100 times.
All inputs are finite; a program needn't handle non-finite values.
Results may differ from the reference program's by a relative error of at most 0.01.
Values may be sent and summed in bfloat16 or wider, within the bound.
A program may use at most 128 MiB of HBM per device.

```python
import math
import jax
import jax.numpy as jnp
import numpy as np
from jax import lax

D = 2048
HEADS = 8
HD = 128
FFE = 3072
TOPK = 2
TA = 256
TB = 384
SEQUENCE_TOKENS = 2048
TOKB = 3072
EXPERTS = 8
CAP = 100
N_EP = 8
N_TP = 4


def plant_pair(key):
    base = jax.random.fold_in(key, 7)
    key_query, key_key = jax.random.split(base, 2)
    width = HEADS * HD
    queries = jnp.clip(1.7 * jax.random.normal(key_query, (SEQUENCE_TOKENS, width), jnp.float32), -5.0, 5.0)
    keys = jnp.clip(jax.random.normal(key_key, (SEQUENCE_TOKENS, width), jnp.float32), -5.0, 5.0)
    return (queries, keys)


def draw_queries(key, part):
    return plant_pair(key)[0].astype(jnp.bfloat16)


def draw_keys(key, part):
    return plant_pair(key)[1].astype(jnp.bfloat16)


def draw_gate_totals(key, part):
    key_portions = jax.random.split(jax.random.fold_in(key, 13), 7)
    order = jax.random.permutation(key_portions[0], HEADS)
    fast = (order < HEADS // 2).astype(jnp.float32)
    slow_total = jax.random.uniform(key_portions[1], (HEADS,), jnp.float32, 0.15, 0.5)
    reach = jnp.exp(jax.random.uniform(key_portions[2], (HEADS,), jnp.float32, math.log(30.0), math.log(100.0)))
    rate = fast / reach + (1.0 - fast) * slow_total / SEQUENCE_TOKENS
    device_factor = jnp.exp(jax.random.uniform(key_portions[3], (SEQUENCE_TOKENS // TA, HEADS), jnp.float32, -0.7, 0.7))
    rough = jax.random.uniform(key_portions[4], (SEQUENCE_TOKENS, HEADS), jnp.float32, 0.4, 1.6)
    log_steps = -rate[None, :] * jnp.repeat(device_factor, TA, axis=0) * rough
    arrival_rows = jax.random.randint(key_portions[5], (2,), 0, SEQUENCE_TOKENS)
    depth = jax.random.uniform(key_portions[6], (2, HEADS), jnp.float32, 0.22, 0.69)
    expert_matches = (jnp.arange(SEQUENCE_TOKENS)[:, None] == arrival_rows[None, :]).astype(jnp.float32)
    log_steps = log_steps - jnp.dot(expert_matches, depth) * (1.0 - fast)[None, :]
    return jnp.cumsum(log_steps, axis=0)


def draw_moe_input(key, part):
    key_main = jax.random.fold_in(jax.random.fold_in(key, 17), 0)
    result = jnp.clip(jax.random.normal(key_main, (TOKB, D), jnp.float32), -6.0, 6.0)
    return result.astype(jnp.bfloat16)


def block_levels(own_key, extent, shards, low, high):
    def one(position, blocks):
        steps = jax.random.uniform(jax.random.fold_in(jax.random.fold_in(own_key, 6), position), (blocks,), jnp.float32, low / len(shards), high / len(shards))
        return jnp.repeat(jnp.exp(steps), extent[position] // blocks).reshape((-1,) + (1,) * (len(extent) - position - 1))

    gain = one(*shards[0])
    for cut in shards[1:]:
        gain = gain * one(*cut)
    return gain


def deal_out(key, own, number, rows, number_of, top, most, slope):
    order = jax.random.permutation(key, number_of)
    packed, ordinary = load_shares(number_of, rows * top, most, slope, True), load_shares(number_of, rows * top, most, slope, False)
    places = jnp.arange(number_of)

    def named(tallies, turn):
        used = int((tallies > 0).sum())
        fixed = max(1, used // 4)
        moved = fixed + (places - fixed + turn * (used - fixed)) % max(1, number_of - fixed)
        return jnp.zeros((number_of,), jnp.int32).at[order[jnp.where(places < fixed, places, moved)]].set(jnp.asarray(tallies, jnp.int32))

    tallies = jnp.where(number % 4 == 0, named(packed, number // 4), named(ordinary, number - number // 4 - 1))
    mixed = jax.random.permutation(jax.random.fold_in(own, 3), number_of)
    source_of, sink = mixed[0:number_of // 2 * 2:2], mixed[1:number_of // 2 * 2:2]
    room = jnp.minimum(tallies[source_of] - 1, most - tallies[sink]) // 2
    room = jnp.where((source_of == order[0]) | (sink == order[0]) | (tallies[sink] == 0), 0, jnp.maximum(room, 0))
    moved = jax.random.randint(jax.random.fold_in(own, 4), (number_of // 2,), 0, 1 << 20) % (room + 1)
    tallies = tallies.at[source_of].add(-moved).at[sink].add(moved)
    labels = jnp.searchsorted(jnp.cumsum(tallies), jnp.arange(rows * top), side="right").astype(jnp.int32)
    listing = labels.reshape(top, rows).T
    listing = listing[jax.random.permutation(jax.random.fold_in(own, 1), rows)]
    turn = jax.random.randint(jax.random.fold_in(own, 2), (rows, 1), 0, top)
    return jnp.take_along_axis(listing, (jnp.arange(top)[None, :] + turn) % top, axis=1)


def load_shares(amount, total, limit, skew, full):
    portions = [(1 << 20) // math.isqrt(rank ** skew) + 1 for rank in range(1, amount + 1)]
    largest = limit if full else min(limit, max(-(-total // amount), total * portions[0] // sum(portions)))
    least = 1 if total - largest >= amount - 1 else 0
    counts, surplus = [largest] + [least] * (amount - 1), total - largest - least * (amount - 1)
    while surplus > 0:
        movable = [i for i in range(1, amount) if counts[i] < largest] or [i for i in range(1, amount) if counts[i] < limit]
        whole, budget = sum([portions[i] for i in movable]), surplus
        for i in movable:
            more = min(limit - counts[i], max(1, budget * portions[i] // whole), surplus)
            counts[i] = counts[i] + more
            surplus = surplus - more
    return np.array(counts)


def centred(key, shape, scale, limit, cuts=(), kind=jnp.bfloat16):
    gain = block_levels(key, shape, cuts, -0.22, 0.18) if cuts else 1.0
    values = jax.random.normal(key, shape, jnp.float32) * scale * gain
    return jnp.minimum(jnp.maximum(values, -limit), limit).astype(kind)


def setup_inputs(seed: int = 0) -> dict:
    key_of = jax.random.split(jax.random.key(seed), 13)
    queries = draw_queries(jax.random.fold_in(key_of[12], 71), 0)
    keys = draw_keys(jax.random.fold_in(key_of[12], 71), 0)
    values = centred(key_of[2], (SEQUENCE_TOKENS, HEADS * HD), 1.0, 6.0, ((0, 8), (1, 4)))
    gate_totals = draw_gate_totals(jax.random.fold_in(key_of[12], 71), 0)
    out_proj = centred(key_of[4], (HEADS * HD, D), (HEADS * HD // 16) ** -0.5, 0.75, ((0, 4),))
    moe_input = draw_moe_input(jax.random.fold_in(key_of[12], 71), 0)
    norm_gain = jnp.clip(1.0 + 0.18 * jax.random.normal(key_of[6], (D,), jnp.float32), 0.1, 1.9)
    routes_keys = jax.random.split(jax.random.fold_in(key_of[7], 1), TOKB // TB)
    routes_turns = jax.random.permutation(jax.random.fold_in(key_of[7], 3), TOKB // TB)
    routes = jax.vmap(lambda own, number: deal_out(jax.random.fold_in(key_of[7], 2), own, number, TB, EXPERTS, TOPK, CAP, 1))(routes_keys, routes_turns).reshape((TOKB, TOPK))
    route_logits = centred(key_of[8], (TOKB, TOPK), 1.5, 6.0, ((0, 8),), jnp.float32)
    expert_gate = centred(key_of[9], (EXPERTS, D, FFE), D ** -0.5, 0.125, ((0, 8), (2, 4)))
    expert_up = centred(key_of[10], (EXPERTS, D, FFE), D ** -0.5, 0.125, ((0, 8), (2, 4)))
    expert_down = centred(key_of[11], (EXPERTS, FFE, D), FFE ** -0.5, 0.109375, ((0, 8), (1, 4)))
    return {"queries": queries, "keys": keys, "values": values, "gate_totals": gate_totals, "out_proj": out_proj, "moe_input": moe_input, "norm_gain": norm_gain, "routes": routes, "route_logits": route_logits, "expert_gate": expert_gate, "expert_up": expert_up, "expert_down": expert_down}


epsilon = 1e-06

def attention_per_head(head_queries, head_keys, value_per_head, head_totals):
    block = math.gcd(SEQUENCE_TOKENS, 512)
    scale = 1.0 / math.sqrt(HD)
    key_pos = jnp.arange(SEQUENCE_TOKENS, dtype=jnp.int32)

    def one_block(index):
        start = (index * block).astype(jnp.int32)
        query_block = lax.dynamic_slice_in_dim(head_queries, start, block, 0)
        total_block = lax.dynamic_slice_in_dim(head_totals, start, block, 0)
        scores = jnp.dot(query_block, head_keys.T, preferred_element_type=jnp.float32) * scale
        scores = scores + total_block[:, None] - head_totals[None, :]
        query_pos = start + jnp.arange(block, dtype=jnp.int32)
        scores = jnp.where(key_pos[None, :] <= query_pos[:, None], scores, -jnp.inf)
        weights = jnp.exp(scores - lax.optimization_barrier(jnp.max(scores, axis=1, keepdims=True)))
        denominator = lax.optimization_barrier(jnp.sum(weights, axis=1, keepdims=True))
        summed = jnp.dot(weights.astype(jnp.bfloat16), value_per_head, preferred_element_type=jnp.float32)
        return (summed / denominator).astype(jnp.bfloat16)
    return lax.map(one_block, jnp.arange(SEQUENCE_TOKENS // block, dtype=jnp.int32)).reshape(SEQUENCE_TOKENS, HD)

def split_heads(array):
    return jnp.transpose(array.reshape(SEQUENCE_TOKENS, HEADS, HD), (1, 0, 2))

def reference(queries, keys, values, gate_totals, out_proj, moe_input, norm_gain, routes, route_logits, expert_gate, expert_up, expert_down):

    def one_head(parts):
        return attention_per_head(parts[0], parts[1], parts[2], parts[3])
    head_mix = lax.map(one_head, (split_heads(queries), split_heads(keys), split_heads(values), jnp.transpose(gate_totals)))
    group = HEADS // N_TP
    head_weights = out_proj.reshape(HEADS, HD, D)
    mixed_total = jnp.zeros((SEQUENCE_TOKENS, D), jnp.float32)
    for index in range(N_TP):
        part = jnp.einsum('hqd,hdn->qn', head_mix[index * group:(index + 1) * group].astype(jnp.float32), head_weights[index * group:(index + 1) * group].astype(jnp.float32))
        mixed_total = mixed_total + lax.optimization_barrier(part.astype(jnp.bfloat16)).astype(jnp.float32)
    mixed = mixed_total.astype(jnp.bfloat16)
    moe_float = moe_input.astype(jnp.float32)
    normed = (moe_float * lax.rsqrt(lax.optimization_barrier(jnp.mean(moe_float * moe_float, axis=1, keepdims=True)) + epsilon) * norm_gain).astype(jnp.bfloat16)
    flat_routes = routes.reshape(N_EP, TB * TOPK)
    indicator_matrix = (flat_routes[:, :, None] == jnp.arange(EXPERTS, dtype=jnp.int32)[None, None, :]).astype(jnp.int32)
    rank = lax.optimization_barrier(jnp.sum((jnp.cumsum(indicator_matrix, axis=1) - indicator_matrix) * indicator_matrix, axis=2))
    source_dev = jnp.arange(N_EP, dtype=jnp.int32)[:, None]
    slot_of = (flat_routes * (N_EP * CAP) + source_dev * CAP + rank).reshape(-1).astype(jnp.int32)
    token_of = (source_dev * TB + jnp.arange(TB * TOPK, dtype=jnp.int32)[None, :] // TOPK).reshape(-1).astype(jnp.int32)
    source = jnp.full((EXPERTS * N_EP * CAP,), TOKB, jnp.int32).at[slot_of].set(token_of)
    padded = jnp.concatenate([normed, jnp.zeros((1, D), jnp.bfloat16)], axis=0)
    quarter = FFE // N_TP

    def one_expert(expert):
        chosen = lax.dynamic_slice_in_dim(source, (expert * (N_EP * CAP)).astype(jnp.int32), N_EP * CAP, 0)
        rows = jnp.take(padded, chosen, axis=0)
        gate_rows = jnp.dot(rows, expert_gate[expert], preferred_element_type=jnp.float32)
        up_rows = jnp.dot(rows, expert_up[expert], preferred_element_type=jnp.float32)
        hidden = (jax.nn.silu(gate_rows) * up_rows).astype(jnp.bfloat16)
        down = expert_down[expert]
        total = jnp.zeros((N_EP * CAP, D), jnp.float32)
        for index in range(N_TP):
            part = jnp.dot(hidden[:, index * quarter:(index + 1) * quarter], down[index * quarter:(index + 1) * quarter], preferred_element_type=jnp.float32)
            total = total + lax.optimization_barrier(part.astype(jnp.bfloat16)).astype(jnp.float32)
        return total.astype(jnp.bfloat16)
    expert_rows = lax.map(one_expert, jnp.arange(EXPERTS, dtype=jnp.int32))
    picked = jnp.take(expert_rows.reshape(EXPERTS * N_EP * CAP, D), slot_of, axis=0).reshape(TOKB, TOPK, D)
    route_weights = jax.nn.sigmoid(route_logits - route_logits[:, ::-1])
    routed = lax.optimization_barrier(jnp.sum(picked.astype(jnp.float32) * route_weights[:, :, None], axis=1)).astype(jnp.bfloat16)
    return (mixed, routed)
```

```python
import functools
import math

import jax
import jax.numpy as jnp
from jax import lax
from jax.experimental import pallas as pl
from jax.experimental.pallas import tpu as pltpu
from jax.sharding import PartitionSpec as P

epsilon = 1e-06
far_below = -1e30
f32 = jnp.float32
bf16 = jnp.bfloat16


def attention_kernel(heads, span, spans, start_ref, q_ref, k_ref, v_ref, qt_ref, kt_ref, w_ref, out_ref, mix_ref):
    rows = q_ref.shape[0]
    hd = q_ref.shape[1] // heads
    scale = 1.0 / math.sqrt(hd)
    first = start_ref[0]
    step_rows = min(rows, 128)
    for h in range(heads):
        cols = slice(h * hd, (h + 1) * hd)
        for r in range(rows // step_rows):
            rsl = slice(r * step_rows, (r + 1) * step_rows)
            q = q_ref[rsl, cols]
            qt = qt_ref[rsl, h : h + 1]
            row_pos = first + r * step_rows + lax.broadcasted_iota(jnp.int32, (step_rows, 1), 0)

            def one(i, carry, q=q, qt=qt, row_pos=row_pos, cols=cols, h=h):
                top, total, acc = carry
                at = pl.multiple_of(i * span, span)
                k = k_ref[pl.ds(at, span), cols]
                v = v_ref[pl.ds(at, span), cols]
                s = lax.dot_general(q, k, (((1,), (1,)), ((), ())), preferred_element_type=f32) * scale
                s = s + qt - kt_ref[h : h + 1, pl.ds(at, span)]
                pos = at + lax.broadcasted_iota(jnp.int32, (1, span), 1)
                s = jnp.where(pos <= row_pos, s, far_below)
                new = jnp.maximum(top, jnp.max(s, axis=1, keepdims=True))
                w = jnp.where(pos <= row_pos, jnp.exp(s - new), 0.0)
                shrink = jnp.exp(top - new)
                total = total * shrink + jnp.sum(w, axis=1, keepdims=True)
                acc = acc * shrink + jnp.dot(w.astype(bf16), v, preferred_element_type=f32)
                return new, total, acc

            init = (
                jnp.full((step_rows, 1), far_below, f32),
                jnp.zeros((step_rows, 1), f32),
                jnp.zeros((step_rows, hd), f32),
            )
            _, total, acc = lax.fori_loop(0, spans, one, init)
            mix_ref[rsl, cols] = (acc / total).astype(bf16)
    out_ref[...] = jnp.dot(mix_ref[...], w_ref[...], preferred_element_type=f32).astype(bf16)


def attention(first_row, queries, keys, values, q_totals, k_totals, out_proj, heads):
    rows, width = queries.shape
    count = keys.shape[0]
    span = math.gcd(count, 1024)
    vm = pl.BlockSpec(memory_space=pltpu.VMEM)
    return pl.pallas_call(
        functools.partial(attention_kernel, heads, span, count // span),
        out_shape=jax.ShapeDtypeStruct((rows, out_proj.shape[1]), bf16),
        in_specs=[pl.BlockSpec(memory_space=pltpu.SMEM)] + [vm] * 6,
        out_specs=vm,
        scratch_shapes=[pltpu.VMEM((rows, width), bf16)],
        compiler_params=pltpu.CompilerParams(vmem_limit_bytes=40 << 20),
        cost_estimate=pl.CostEstimate(
            flops=4_000_000_000, bytes_accessed=4 * count * width, transcendentals=rows * count * heads
        ),
        name="attention",
    )(first_row[None], queries, keys, values, q_totals, k_totals, out_proj)


def three_terms(x):
    hi = lax.reduce_precision(x, 8, 7)
    rest = x - hi
    mid = lax.reduce_precision(rest, 8, 7)
    return jnp.concatenate([hi, mid, rest - mid], axis=1).astype(bf16)


def body(
    queries,
    keys,
    values,
    gate_totals,
    out_proj,
    moe_input,
    norm_gain,
    routes,
    route_logits,
    expert_gate,
    expert_up,
    expert_down,
):
    tok_rows, local_heads = gate_totals.shape
    width = out_proj.shape[1]
    part_width = keys.shape[1]
    tok_b, width_b = moe_input.shape
    top = routes.shape[1]
    ep_count = lax.axis_size("ep")
    tp_count = lax.axis_size("tp")
    capacity = tp_count * (tok_b * top // (tp_count * ep_count) + 1)
    slots = ep_count * capacity
    quarter = width_b // tp_count
    my_tp = lax.axis_index("tp")

    flat = jnp.transpose(routes).reshape(1, top * tok_b)
    chosen = (lax.broadcasted_iota(jnp.int32, (ep_count, 1), 0) == flat).astype(bf16)
    line = lax.iota(jnp.int32, top * tok_b)
    order = (line % tok_b) * top + line // tok_b
    before = (order[:, None] < order[None, :]).astype(bf16)
    counts = jnp.dot(chosen, before, preferred_element_type=f32)
    rank = jnp.sum(counts * chosen.astype(f32), axis=0).astype(jnp.int32)
    slot_of = (flat[0] * capacity + rank).reshape(top, tok_b)
    slot_ids = lax.iota(jnp.int32, slots)
    hits = [slot_of[k][None, :] == slot_ids[:, None] for k in range(top)]
    pick = functools.reduce(jnp.logical_or, hits).astype(bf16)

    moe_float = moe_input.astype(f32)
    mean = jnp.mean(moe_float * moe_float, axis=1, keepdims=True)
    mine = lax.dynamic_slice_in_dim(moe_input, my_tp * quarter, quarter, 1).astype(f32)
    gain = lax.dynamic_slice_in_dim(norm_gain, my_tp * quarter, quarter, 0)
    normed = (mine * lax.rsqrt(mean + epsilon) * gain).astype(bf16)
    outgoing = jnp.dot(pick, normed, preferred_element_type=f32).astype(bf16)
    arrived = lax.all_to_all(
        outgoing.reshape(ep_count, capacity, quarter), "ep", split_axis=0, concat_axis=0, tiled=True
    ).reshape(slots, quarter)

    shared = jnp.concatenate(
        [keys, values, jnp.pad(three_terms(gate_totals), ((0, 0), (0, 128 - 3 * local_heads)))], axis=1
    )
    everyone = lax.all_gather(shared, "ep", axis=0, tiled=True)
    terms = everyone[:, 2 * part_width : 2 * part_width + 3 * local_heads].astype(f32)
    all_totals = (
        terms[:, :local_heads] + terms[:, local_heads : 2 * local_heads] + terms[:, 2 * local_heads :]
    )
    attn_term = attention(
        lax.axis_index("ep") * tok_rows,
        queries,
        everyone[:, :part_width],
        everyone[:, part_width : 2 * part_width],
        gate_totals,
        jnp.transpose(all_totals),
        out_proj,
        local_heads,
    )
    mixed = lax.psum_scatter(attn_term, "tp", scatter_dimension=1, tiled=True)

    rows = lax.all_gather(arrived, "tp", axis=0, tiled=True).reshape(tp_count, slots, quarter)
    gate_w = expert_gate[0].reshape(tp_count, quarter, -1)
    up_w = expert_up[0].reshape(tp_count, quarter, -1)
    gate_rows = sum(jnp.dot(rows[i], gate_w[i], preferred_element_type=f32) for i in range(tp_count))
    up_rows = sum(jnp.dot(rows[i], up_w[i], preferred_element_type=f32) for i in range(tp_count))
    hidden = (jax.nn.silu(gate_rows) * up_rows).astype(bf16)
    unit_term = jnp.dot(hidden, expert_down[0], preferred_element_type=f32).astype(bf16)
    expert_rows = lax.psum_scatter(unit_term, "tp", scatter_dimension=1, tiled=True)
    returned = lax.all_to_all(
        expert_rows.reshape(ep_count, capacity, quarter), "ep", split_axis=0, concat_axis=0, tiled=True
    ).reshape(slots, quarter)

    route_weights = jax.nn.sigmoid(route_logits - route_logits[:, ::-1])
    place = sum(
        jnp.where(slot_of[k][:, None] == slot_ids[None, :], route_weights[:, k : k + 1], 0.0)
        for k in range(top)
    )
    place_hi = lax.reduce_precision(place, 8, 7)
    place_lo = (place - place_hi).astype(bf16)
    routed = (
        jnp.dot(place_hi.astype(bf16), returned, preferred_element_type=f32)
        + jnp.dot(place_lo, returned, preferred_element_type=f32)
    ).astype(bf16)
    return (mixed, routed)


def solution(mesh):
    return jax.shard_map(
        body,
        mesh=mesh,
        in_specs=(
            P("ep", "tp"),
            P("ep", "tp"),
            P("ep", "tp"),
            P("ep", "tp"),
            P("tp", None),
            P("ep", None),
            P(),
            P("ep", None),
            P("ep", None),
            P("ep", None, "tp"),
            P("ep", None, "tp"),
            P("ep", "tp", None),
        ),
        out_specs=(P("ep", "tp"), P("ep", "tp")),
        check_vma=False,
    )
```
